32 devices in a mesh: grp: 2 (over x), ep: 16 (over z, y, core).
Axes of the slice: x: 2, y: 2, z: 4, core: 2. Of those that a mesh axis runs over, the one named last changes fastest.
Arguments:
- tokens: bfloat16 [4096, 2048], P(('grp', 'ep')), parts along dimension 0, may hold values from -6 to 6
- norm_gain: float32 [2048], replicated, may hold values from 0.1 to 1.9
- expert_ids: int32 [4096, 2], P(('grp', 'ep')), parts along dimension 0, may hold values from 0 to 3, as said below
- mix_weights: float32 [4096, 2], P(('grp', 'ep')), parts along dimension 0, may hold values from 0.2 to 1
- gate_weight: bfloat16 [2048, 28672], P(None, 'ep'), may hold values from -0.125 to 0.125
- up_weight: bfloat16 [2048, 28672], P(None, 'ep'), may hold values from -0.125 to 0.125
- down_weight: bfloat16 [28672, 2048], P('ep'), may hold values from -0.0625 to 0.0625
Outputs:
- mixed: bfloat16 [4096, 2048], P(('grp', 'ep')), parts along dimension 0
The draws below stay inside these ranges and needn't reach their ends.
There are 2 independent parts, one for each index of `grp`. The reference program is written for one: setup_inputs(seed, part) draws one part's arguments, and reference() takes and returns one part's arrays. A program takes and returns all parts, laid end to end along the dimension named above; an argument that names none is the same for every part. Nothing has to cross between parts.
Inputs may be any that keep to these rules, and one draw needn't show every extreme that they name: `expert_ids`: each token names 2 different experts. In the rows of one device no expert is named by more than 80 rows, and in every draw each expert is named by exactly 80 rows of some device.
All inputs are finite; a program needn't handle non-finite values.
Results may differ from the reference program's by a relative error of at most 0.008.
Values may be sent and summed in bfloat16 or wider, within the bound.
A program may use at most 128 MiB of HBM per device.

```python
import jax
import jax.numpy as jnp
from jax import lax

D = 2048
FF = 7168
TOP = 2
SPLIT = 4
TOK_DEV = 128
EXPERTS = 4
CAP = 80
TOKENS = 2048
N_EP = 16


def draw_expert_ids(key, part):
    key_shift = jax.random.fold_in(key, 11)
    key_offset = jax.random.fold_in(key, 12)
    key_order = jax.random.fold_in(key, 13)
    key_swap = jax.random.fold_in(key, 14)
    shift = jax.random.randint(key_shift, (), 0, EXPERTS)
    blocks = jnp.arange(N_EP, dtype=jnp.int32)
    favoured = ((blocks + shift) % EXPERTS)[:, None]
    positions = jnp.arange(TOK_DEV, dtype=jnp.int32)
    chosen = positions < CAP
    picks_before = jnp.where(chosen, positions, CAP + 2 * (positions - CAP))[None, :]
    offsets = jax.random.randint(key_offset, (N_EP, 1), 0, EXPERTS - 1)
    first_other = (picks_before + offsets) % (EXPERTS - 1)
    second_other = (picks_before + 1 + offsets) % (EXPERTS - 1)
    first_expert = (favoured + 1 + first_other) % EXPERTS
    second_expert = (favoured + 1 + second_other) % EXPERTS
    column_one = jnp.where(chosen[None, :], favoured, first_expert)
    column_two = jnp.where(chosen[None, :], first_expert, second_expert)
    orders = jax.vmap(lambda k: jax.random.permutation(k, TOK_DEV))(jax.random.split(key_order, N_EP))
    column_one = jnp.take_along_axis(column_one, orders, axis=1)
    column_two = jnp.take_along_axis(column_two, orders, axis=1)
    flips = jax.random.randint(key_swap, (N_EP, TOK_DEV), 0, 2)
    left = jnp.where(flips == 1, column_two, column_one)
    right = jnp.where(flips == 1, column_one, column_two)
    paired = jnp.stack([left, right], axis=2)
    return paired.reshape(TOKENS, TOP).astype(jnp.int32)


def steps_of(own_key, extent, shards, low, high):
    level = 1.0
    for position, shards_of in shards:
        heights = jax.random.uniform(jax.random.fold_in(jax.random.fold_in(own_key, 6), position), (shards_of,), jnp.float32, low / len(shards), high / len(shards))
        level = level * jnp.repeat(jnp.exp(heights), extent[position] // shards_of).reshape((-1,) + (1,) * (len(extent) - 1 - position))
    return level


def scatter_about(stream_key, dims, spread, most, pieces=(), kind=jnp.bfloat16):
    entries = spread * jax.random.normal(stream_key, dims, jnp.float32)
    if pieces:
        entries = entries * steps_of(stream_key, dims, pieces, -0.22, 0.18)
    return jnp.clip(entries, -most, most).astype(kind)


def setup_inputs(seed: int = 0, part: int = 0) -> dict:
    key_of = jax.random.split(jax.random.key(seed), 8)
    own_keys = jax.random.split(jax.random.fold_in(key_of[7], part), 8)
    return {
        "tokens": scatter_about(own_keys[0], (TOKENS, D), 1.0, 6.0, ((0, 16),)),
        "norm_gain": jnp.clip(1.0 + 0.18 * jax.random.normal(key_of[1], (D,), jnp.float32), 0.1, 1.9),
        "expert_ids": draw_expert_ids(jax.random.fold_in(jax.random.fold_in(key_of[7], part), 71), part),
        "mix_weights": jnp.clip(0.2 + 0.8 * jax.random.uniform(own_keys[3], (TOKENS, TOP), jnp.float32) ** steps_of(own_keys[3], (TOKENS, TOP), ((0, 16),), -0.2, 0.2), 0.2, 1.0),
        "gate_weight": scatter_about(key_of[4], (D, EXPERTS * FF), D ** -0.5, 0.125, ((1, 16),)),
        "up_weight": scatter_about(key_of[5], (D, EXPERTS * FF), D ** -0.5, 0.125, ((1, 16),)),
        "down_weight": scatter_about(key_of[6], (EXPERTS * FF, D), FF ** -0.5, 0.0625, ((0, 16),)),
    }


def block_slots(ids):
    flat = ids.reshape(-1)
    onehot = (flat[:, None] == jnp.arange(EXPERTS, dtype=jnp.int32)[None, :]).astype(jnp.int32)
    before = jnp.cumsum(onehot, axis=0) - onehot
    return lax.optimization_barrier(jnp.sum(before * onehot, axis=1)).reshape(ids.shape)

def reference(tokens, norm_gain, expert_ids, mix_weights, gate_weight, up_weight, down_weight):
    values = tokens.astype(jnp.float32)
    normed = (values * lax.rsqrt(lax.optimization_barrier(jnp.mean(values * values, axis=-1, keepdims=True)) + 1e-06) * norm_gain).astype(jnp.bfloat16)
    ids = expert_ids.reshape(N_EP, TOK_DEV, TOP)
    slots = jax.vmap(block_slots)(ids)
    source = jnp.broadcast_to(jnp.arange(N_EP, dtype=jnp.int32)[:, None, None], ids.shape)
    rows = jnp.broadcast_to(normed.reshape(N_EP, TOK_DEV, 1, D), (N_EP, TOK_DEV, TOP, D))
    buffers = jnp.zeros((EXPERTS, N_EP, CAP, D), jnp.bfloat16)
    buffers = buffers.at[ids, source, slots].set(rows)
    slice_width = FF // SPLIT

    def one_expert(args):
        expert, block = args
        inputs = block.reshape(N_EP * CAP, D)
        total = jnp.zeros((N_EP * CAP, D), jnp.float32)
        for part in range(SPLIT):
            start = (expert * FF + part * slice_width).astype(jnp.int32)
            w_gate = lax.dynamic_slice_in_dim(gate_weight, start, slice_width, 1)
            w_up = lax.dynamic_slice_in_dim(up_weight, start, slice_width, 1)
            w_down = lax.dynamic_slice_in_dim(down_weight, start, slice_width, 0)
            gate = jnp.dot(inputs, w_gate, preferred_element_type=jnp.float32)
            upper = jnp.dot(inputs, w_up, preferred_element_type=jnp.float32)
            hidden = (jax.nn.silu(gate) * upper).astype(jnp.bfloat16)
            partial_out = jnp.dot(hidden, w_down, preferred_element_type=jnp.float32).astype(jnp.bfloat16)
            total = total + partial_out.astype(jnp.float32)
        return total.reshape(N_EP, CAP, D)
    expert_out = lax.map(one_expert, (jnp.arange(EXPERTS, dtype=jnp.int32), buffers))
    picked = expert_out[ids, source, slots]
    mixed = lax.optimization_barrier(jnp.sum(mix_weights.reshape(N_EP, TOK_DEV, TOP, 1) * picked, axis=2))
    return mixed.reshape(TOKENS, D).astype(jnp.bfloat16)
```

```python
import functools

import jax
import jax.numpy as jnp
from jax import lax
from jax.experimental import pallas as pl
from jax.experimental.pallas import tpu as pltpu
from jax.sharding import PartitionSpec as P

SPLIT = 4
CHUNK = 16
f32, bf16 = jnp.float32, jnp.bfloat16


def tile_of(extent, most):
    tile = most
    while extent % tile:
        tile //= 2
    return tile


def cut(extent):
    first = (extent // 256 + 1) // 2 * 256
    return ((0, first), (first, extent - first))


def plan(experts, nq):
    last = experts - 1
    sides = []
    for inner in (False, True):
        ev = {}

        def at(step, place, *items, ev=ev):
            ev.setdefault((step, place), []).extend(items)

        if experts == 4:
            half = (nq + 1) // 2
            if inner:
                at(0, 1, ("z", 2, 0, nq))
                at(0, 2, ("y", 1, 0, nq - 1))
                at(0, 3, ("y", 1, nq - 1, nq))
                at(0, 4, ("z", 3, 0, half - 1))
                at(1, 1, ("z", 3, half - 1, half))
                at(1, 2, ("z", 3, half, half + 1))
                at(1, 3, ("z", 3, half + 1, nq), ("y", 2, 0, nq))
                at(2, 1, ("chip", 1, 0, nq))
                at(2, 3, ("y", 3, 0, nq))
                at(3, 1, ("group", 1, 0, half), ("chip", 0, 0, half))
                at(3, 2, ("group", 1, half, nq))
                tail = [
                    ("chip", 3, 0, nq), ("chip", 2, 0, nq), ("chip", 0, half, nq),
                    ("group", 0, 0, half), ("group", 3, 0, nq), ("mix", 1), ("group", 2, 0, nq),
                    ("mix", 2), ("group", 0, half, nq), ("mix", 0), ("mix", 3),
                ]
            else:
                at(0, 1, ("z", 2, 0, 1))
                at(0, 2, ("z", 2, 1, 2), ("y", 1, 0, nq - 1))
                at(0, 3, ("y", 1, nq - 1, nq))
                at(0, 4, ("z", 2, 2, half))
                at(1, 1, ("z", 2, half, half + 1))
                at(1, 3, ("z", 2, half + 1, nq))
                at(1, 4, ("z", 3, 0, 1), ("y", 2, 0, nq))
                at(2, 1, ("z", 3, 1, half))
                at(2, 2, ("z", 3, half, nq))
                at(2, 3, ("chip", 0, 0, half))
                at(2, 4, ("y", 3, 0, nq))
                at(3, 1, ("chip", 2, 0, nq))
                at(3, 2, ("group", 0, 0, half))
                tail = [
                    ("chip", 3, 0, nq), ("chip", 1, 0, nq), ("chip", 0, half, nq),
                    ("group", 2, 0, nq), ("group", 3, 0, nq), ("mix", 1), ("group", 1, 0, nq),
                    ("mix", 2), ("group", 0, half, nq), ("mix", 0), ("mix", 3),
                ]
        else:
            for k in range(experts):
                if k + 2 < experts:
                    at(k, 2, ("z", k + 2, 0, nq))
                if k + 1 < experts:
                    at(k, 4, ("y", k + 1, 0, nq))
                if k > 0:
                    at(k, 1, ("chip", k - 1, 0, nq))
                    at(k, 3, ("group", k - 1, 0, nq))
            tail = [("chip", last, 0, nq), ("group", last, 0, nq)] + [("mix", k) for k in range(experts)]
        sides.append((ev, tail))
    return sides


def kernel(
    experts,
    tok_ref, gain_ref, ids_ref, mix_ref, wg_hbm, wu_hbm, wd_hbm,
    out_ref,
    wg, wu, wd, normed, disp, xin, hid, part, r1, r2s, r2r, r3s, home, acc,
    w_sem, zs_sem, zr_sem, ys_sem, yr_sem, cs_sem, cr_sem, ds_sem, dr_sem,
    r1s_sem, r1r_sem, r2s_sem, r2r_sem, r3s_sem, r3r_sem,
):
    me = lax.axis_index("ep")
    z = me // SPLIT
    y = (me // 2) % 2
    c = me % 2
    rows, width = tok_ref.shape
    cap = disp.shape[1]
    nq = cap // CHUNK
    ff = wg.shape[1]
    top = ids_ref.shape[0]
    at_y = {"ep": z * SPLIT + (1 - y) * 2 + c}
    at_c = {"ep": z * SPLIT + y * 2 + (1 - c)}
    mine = c * 2 + y
    other_y = c * 2 + 1 - y
    other_c = (1 - c) * 2 + y
    other_yc = (1 - c) * 2 + 1 - y
    near = jnp.minimum(z, experts - 1 - z)
    away = jnp.where(2 * z < experts, 1, -1)
    inner = near > 0
    edge = near == 0

    def peer(k):
        both = z + away * ((k + 1) // 2) * (2 * (k % 2) - 1)
        return jnp.where(k <= 2 * near, both, z + away * (k - near))

    def at_z(k):
        return {"ep": peer(k) * SPLIT + y * 2 + c}

    def remote(src, dst, send, recv, where):
        return pltpu.make_async_remote_copy(
            src_ref=src, dst_ref=dst, send_sem=send, recv_sem=recv,
            device_id=where, device_id_type=pl.DeviceIdType.MESH,
        )

    def chunk(q):
        return pl.ds(pl.multiple_of(q * CHUNK, CHUNK), CHUNK)

    ff_cuts = cut(ff)
    out_cuts = cut(width)
    pieces = w_sem.shape[1]

    def weight(which):
        hbm, vmem = ((wg_hbm, wg), (wu_hbm, wu), (wd_hbm, wd))[which]
        size = hbm.shape[0] // pieces
        return [
            pltpu.make_async_copy(
                hbm.at[pl.ds(i * size, size)], vmem.at[pl.ds(i * size, size)], w_sem.at[which, i]
            )
            for i in range(pieces)
        ]

    barrier = pltpu.get_barrier_semaphore()
    for k in range(1, experts):
        pl.semaphore_signal(barrier, inc=1, device_id=at_z(k), device_id_type=pl.DeviceIdType.MESH)
    pl.semaphore_signal(barrier, inc=1, device_id=at_y, device_id_type=pl.DeviceIdType.MESH)
    pl.semaphore_signal(barrier, inc=1, device_id=at_c, device_id_type=pl.DeviceIdType.MESH)

    for which in range(3):
        for copy in weight(which):
            copy.start()

    step = tile_of(rows, 32)

    @pl.loop(0, rows // step)
    def _(r):
        at = pl.ds(pl.multiple_of(r * step, step), step)
        values = tok_ref[at, :].astype(f32)
        scale = lax.rsqrt(jnp.mean(values * values, axis=-1, keepdims=True) + 1e-06)
        normed[at, :] = (values * scale * gain_ref[...]).astype(bf16)

    lanes = 128
    expert_row = lax.broadcasted_iota(jnp.int32, (lanes, rows), 0)
    named = ids_ref[0:1, :] == expert_row
    weight_t = jnp.where(named, mix_ref[0:1, :], 0.0)
    for k in range(1, top):
        hit = ids_ref[k : k + 1, :] == expert_row
        named = named | hit
        weight_t = weight_t + jnp.where(hit, mix_ref[k : k + 1, :], 0.0)
    named = named.astype(f32)
    first = lax.broadcasted_iota(jnp.int32, (rows, rows), 0)
    second = lax.broadcasted_iota(jnp.int32, (rows, rows), 1)
    upper = (first < second).astype(f32).astype(bf16)
    rank_t = jnp.dot(named.astype(bf16), upper, preferred_element_type=f32)
    rank_t = jnp.where(named > 0.5, rank_t, -1.0)
    rank = jnp.transpose(rank_t)
    weight_c = jnp.transpose(weight_t)
    lane = lax.broadcasted_iota(jnp.int32, (rows, lanes), 1)

    def dispatch(e, dst):
        slot = jnp.sum(jnp.where(expert_row == e, rank_t, 0.0), axis=0, keepdims=True)
        place = lax.broadcasted_iota(jnp.int32, (cap, rows), 0)
        pick = (place == slot.astype(jnp.int32)).astype(f32).astype(bf16)
        wide = tile_of(width, 512)
        for n in range(width // wide):
            cols = slice(n * wide, (n + 1) * wide)
            dst[:, cols] = jnp.dot(pick, normed[:, cols], preferred_element_type=f32).astype(bf16)

    def z_copy(k, q):
        return remote(disp.at[k, chunk(q)], xin.at[z, mine, chunk(q)], zs_sem.at[k, q], zr_sem.at[z, q], at_z(k))

    def z_arrival(k, q):
        p = peer(k)
        return remote(disp.at[k, chunk(q)], xin.at[p, mine, chunk(q)], zs_sem.at[k, q], zr_sem.at[p, q], at_z(k))

    def in_group(sub, send, recv, where):
        def make(k, q):
            slot = xin.at[peer(k), sub, chunk(q)]
            return remote(slot, slot, send.at[k, q], recv.at[k, q], where)

        return make

    y_copy = in_group(mine, ys_sem, yr_sem, at_y)
    y_arrival = in_group(other_y, ys_sem, yr_sem, at_y)
    c_copy = in_group(mine, cs_sem, cr_sem, at_c)
    c_arrival = in_group(other_c, cs_sem, cr_sem, at_c)
    d_copy = in_group(other_y, ds_sem, dr_sem, at_c)
    d_arrival = in_group(other_yc, ds_sem, dr_sem, at_c)

    def r1_copy(k, v, h):
        start, size = out_cuts[h]
        cols = pl.ds(start, size)
        return remote(
            part.at[k, 1 - c, v, :, cols], r1.at[k, v, :, cols], r1s_sem.at[k, v, h], r1r_sem.at[k, v, h], at_c
        )

    def r2_copy(k, q):
        return remote(r2s.at[k, chunk(q)], r2r.at[k, chunk(q)], r2s_sem.at[k, q], r2r_sem.at[k, q], at_y)

    def r3_copy(k, q):
        return remote(r3s.at[k, chunk(q)], home.at[z, chunk(q)], r3s_sem.at[k, q], r3r_sem.at[z, q], at_z(k))

    def r3_arrival(k, q):
        p = peer(k)
        return remote(r3s.at[k, chunk(q)], home.at[p, chunk(q)], r3s_sem.at[k, q], r3r_sem.at[p, q], at_z(k))

    def forward_z(k, q):
        if k > 0:
            z_arrival(k, q).wait_recv()
        y_copy(k, q).start()
        c_copy(k, q).start()

    def forward_y(k, q):
        y_arrival(k, q).wait_recv()
        d_copy(k, q).start()

    def chip_sum(k, q):
        at = chunk(q)

        @pl.when(q == 0)
        def _():
            for h in range(2):
                r1_copy(k, 1 - y, h).wait_recv()

        r2s[k, at, :] = (part[k, c, 1 - y, at, :].astype(f32) + r1[k, 1 - y, at, :].astype(f32)).astype(bf16)
        r2_copy(k, q).start()

    def group_sum(k, q):
        at = chunk(q)

        @pl.when(q == 0)
        def _():
            for h in range(2):
                r1_copy(k, y, h).wait_recv()

        r2_copy(k, q).wait_recv()
        total = (
            part[k, c, y, at, :].astype(f32) + r1[k, y, at, :].astype(f32) + r2r[k, at, :].astype(f32)
        ).astype(bf16)
        if k == 0:
            home[z, at, :] = total
        else:
            r3s[k, at, :] = total
            r3_copy(k, q).start()

    def mix(k):
        e = peer(k)
        if k > 0:
            @pl.loop(0, nq)
            def _(q):
                r3_arrival(k, q).wait_recv()

        slot = jnp.sum(jnp.where(lane == e, rank, 0.0), axis=1, keepdims=True)
        share = jnp.sum(jnp.where(lane == e, weight_c, 0.0), axis=1, keepdims=True)
        place = lax.broadcasted_iota(jnp.int32, (rows, cap), 1)
        pick = (place == slot.astype(jnp.int32)).astype(f32).astype(bf16)
        wide = tile_of(width, 512)
        for n in range(width // wide):
            cols = slice(n * wide, (n + 1) * wide)
            acc[:, cols] += share * jnp.dot(pick, home[e, :, cols], preferred_element_type=f32)

    actions = {"z": forward_z, "y": forward_y, "chip": chip_sum, "group": group_sum}
    sides = plan(experts, nq)

    def perform(items):
        for item in items:
            if item[0] == "mix":
                mix(item[1])
            else:
                kind, k, lo, hi = item

                @pl.loop(lo, hi)
                def _(q):
                    actions[kind](k, q)

    def service(step_index, place):
        for k in range(experts):
            lists = [side[0].get((k, place), []) for side in sides]
            if lists[0] == lists[1]:
                if lists[0]:
                    @pl.when(step_index == k)
                    def _():
                        perform(lists[0])
            else:
                for items, kind in zip(lists, (edge, inner)):
                    if items:
                        @pl.when((step_index == k) & kind)
                        def _():
                            perform(items)

    dispatch(z, xin.at[z, mine])
    pl.semaphore_wait(barrier, experts + 1)

    @pl.loop(0, nq)
    def _(q):
        forward_z(0, q)

    @pl.loop(1, experts)
    def _(k):
        dispatch(peer(k), disp.at[k])

        @pl.loop(0, nq)
        def _(q):
            z_copy(k, q).start()

    acc[...] = jnp.zeros_like(acc)

    @pl.loop(0, nq)
    def _(q):
        forward_y(0, q)
        if experts > 1:
            forward_z(1, q)

    for which in range(3):
        for copy in weight(which):
            copy.wait()

    @pl.loop(0, experts)
    def _(k):
        @pl.loop(0, nq)
        def _(q):
            c_arrival(k, q).wait_recv()
            d_arrival(k, q).wait_recv()

        for h, (start, size) in enumerate(ff_cuts):
            cols = slice(start, start + size)
            inputs = xin[peer(k)].reshape(SPLIT * cap, width)
            gate = jnp.dot(inputs, wg[:, cols], preferred_element_type=f32)
            up = jnp.dot(inputs, wu[:, cols], preferred_element_type=f32)
            hid[:, cols] = (gate / (1.0 + jnp.exp(-gate)) * up).astype(bf16)
            service(k, 1 + h)

        for h, (start, size) in enumerate(out_cuts):
            cols = slice(start, start + size)
            res = jnp.dot(hid[...], wd[:, cols], preferred_element_type=f32).astype(bf16)
            part[k, :, :, :, cols] = res.reshape(2, 2, cap, size)
            for v in (1 - y, y):
                r1_copy(k, v, h).start()
            service(k, 3 + h)

    tails = [side[1] for side in sides]
    if tails[0] == tails[1]:
        perform(tails[0])
    else:
        for items, kind in zip(tails, (edge, inner)):
            @pl.when(kind)
            def _():
                perform(items)

    out_ref[...] = acc[...].astype(bf16)

    @pl.loop(0, experts)
    def _(k):
        @pl.when(k > 0)
        def _():
            @pl.loop(0, nq)
            def _(q):
                z_copy(k, q).wait_send()
                r3_copy(k, q).wait_send()

        @pl.loop(0, nq)
        def _(q):
            y_copy(k, q).wait_send()
            c_copy(k, q).wait_send()
            d_copy(k, q).wait_send()
            r2_copy(k, q).wait_send()

        for v in range(2):
            for h in range(2):
                r1_copy(k, v, h).wait_send()


def local(tokens, norm_gain, expert_ids, mix_weights, gate_weight, up_weight, down_weight):
    n_dev = lax.axis_size("ep")
    experts = n_dev // SPLIT
    rows, width = tokens.shape
    top = expert_ids.shape[1]
    ff = gate_weight.shape[1]
    cap = (rows * top * SPLIT * 5 + 4 * n_dev - 1) // (4 * n_dev)
    cap = (cap + CHUNK - 1) // CHUNK * CHUNK
    nq = cap // CHUNK
    dma = pltpu.SemaphoreType.DMA
    vmem = pl.BlockSpec(memory_space=pltpu.VMEM)
    hbm = pl.BlockSpec(memory_space=pl.ANY)
    block = (cap, width)
    return pl.pallas_call(
        functools.partial(kernel, experts),
        out_shape=jax.ShapeDtypeStruct((rows, width), bf16),
        in_specs=[vmem, vmem, vmem, vmem, hbm, hbm, hbm],
        out_specs=vmem,
        scratch_shapes=[
            pltpu.VMEM((width, ff), bf16),
            pltpu.VMEM((width, ff), bf16),
            pltpu.VMEM((ff, width), bf16),
            pltpu.VMEM((rows, width), bf16),
            pltpu.VMEM((experts,) + block, bf16),
            pltpu.VMEM((experts, SPLIT) + block, bf16),
            pltpu.VMEM((SPLIT * cap, ff), bf16),
            pltpu.VMEM((experts, 2, 2) + block, bf16),
            pltpu.VMEM((experts, 2) + block, bf16),
            pltpu.VMEM((experts,) + block, bf16),
            pltpu.VMEM((experts,) + block, bf16),
            pltpu.VMEM((experts,) + block, bf16),
            pltpu.VMEM((experts,) + block, bf16),
            pltpu.VMEM((rows, width), f32),
            dma((3, 4)),
        ] + [dma((experts, nq))] * 8 + [dma((experts, 2, 2))] * 2 + [dma((experts, nq))] * 4,
        compiler_params=pltpu.CompilerParams(
            collective_id=0, has_side_effects=True, vmem_limit_bytes=64 * 1024 * 1024 - 65536,
        ),
    )(tokens, norm_gain.reshape(1, width), expert_ids.T, mix_weights.T, gate_weight, up_weight, down_weight)


def solution(mesh):
    in_specs = (
        P(("grp", "ep"), None),
        P(),
        P(("grp", "ep"), None),
        P(("grp", "ep"), None),
        P(None, "ep"),
        P(None, "ep"),
        P("ep", None),
    )
    out_specs = P(("grp", "ep"), None)
    return jax.shard_map(local, mesh=mesh, in_specs=in_specs, out_specs=out_specs, check_vma=False)
```

```python
import functools

import jax
import jax.numpy as jnp
from jax import lax
from jax.experimental import pallas as pl
from jax.experimental.pallas import tpu as pltpu
from jax.sharding import PartitionSpec as P

SPLIT = 4
CHUNK = 16
f32, bf16 = jnp.float32, jnp.bfloat16


def tile_of(extent, most):
    tile = most
    while extent % tile:
        tile //= 2
    return tile


def cut(extent, parts):
    tiles = extent // 256
    ends = [tiles * i // parts * 256 for i in range(parts)] + [extent]
    return tuple((a, b - a) for a, b in zip(ends, ends[1:]))


def plan(experts, nq):
    last = experts - 1
    sides = []
    for inner in (False, True):
        ev = {}

        def at(step, place, *items, ev=ev):
            ev.setdefault((step, place), []).extend(
                (kind, k, nq * lo // 5, nq * hi // 5) for kind, k, lo, hi in items
            )

        if experts == 4:
            if inner:
                at(0, 1, ("z", 2, 0, 5))
                at(0, 3, ("y", 1, 0, 4))
                at(0, 4, ("y", 1, 4, 5))
                at(1, 1, ("chip", 0, 0, 2))
                at(1, 2, ("z", 3, 0, 2))
                at(1, 3, ("z", 3, 2, 3), ("y", 2, 0, 5))
                at(1, 4, ("z", 3, 3, 4))
                at(1, 5, ("z", 3, 4, 5))
                at(2, 1, ("chip", 1, 0, 5), ("y", 3, 0, 2))
                at(2, 3, ("y", 3, 2, 4))
                at(2, 4, ("y", 3, 4, 5))
                at(2, 5, ("group", 1, 0, 2))
                at(3, 1, ("chip", 2, 0, 5), ("group", 1, 2, 3))
                at(3, 2, ("group", 1, 3, 4))
                at(3, 3, ("group", 1, 4, 5))
                at(3, 5, ("group", 2, 0, 2))
                at(4, 0, ("chip", 3, 0, 5), ("chip", 0, 2, 5), ("group", 2, 2, 5), ("group", 3, 0, 5))
                at(4, 0, ("mix", 1, 0, 5), ("group", 0, 0, 5))
                at(4, 0, ("mix", 0, 0, 5), ("mix", 2, 0, 5), ("mix", 3, 0, 5))
            else:
                at(0, 2, ("z", 2, 0, 1))
                at(0, 3, ("z", 2, 1, 2), ("y", 1, 0, 4))
                at(0, 4, ("y", 1, 4, 5), ("z", 2, 2, 4))
                at(0, 5, ("z", 2, 4, 5))
                at(1, 1, ("chip", 0, 0, 2))
                at(1, 4, ("y", 2, 0, 5))
                at(1, 5, ("z", 3, 0, 1))
                at(2, 1, ("z", 3, 1, 2))
                at(2, 2, ("z", 3, 2, 4))
                at(2, 3, ("z", 3, 4, 5), ("chip", 1, 0, 2))
                at(2, 4, ("y", 3, 0, 3))
                at(2, 5, ("y", 3, 3, 5), ("chip", 1, 2, 3))
                at(3, 1, ("chip", 2, 0, 5))
                at(3, 2, ("group", 1, 0, 2))
                at(3, 3, ("group", 2, 0, 1))
                at(3, 4, ("group", 2, 1, 2))
                at(3, 5, ("group", 2, 2, 3))
                at(4, 0, ("chip", 3, 0, 5), ("chip", 1, 3, 5), ("chip", 0, 2, 5), ("group", 2, 3, 5))
                at(4, 0, ("group", 1, 2, 3), ("group", 0, 0, 2), ("group", 3, 0, 5), ("mix", 2, 0, 5))
                at(4, 0, ("group", 1, 3, 5), ("group", 0, 2, 5))
                at(4, 0, ("mix", 0, 0, 5), ("mix", 1, 0, 5), ("mix", 3, 0, 5))
        else:
            for k in range(experts):
                if k + 2 < experts:
                    at(k, 2, ("z", k + 2, 0, 5))
                if k + 1 < experts:
                    at(k, 5, ("y", k + 1, 0, 5))
                if k > 0:
                    at(k, 1, ("chip", k - 1, 0, 5))
                    at(k, 3, ("group", k - 1, 0, 5))
            at(experts, 0, ("chip", last, 0, 5), ("group", last, 0, 5))
            at(experts, 0, *[("mix", k, 0, 5) for k in range(experts)])
        tail = ev.pop((experts, 0))
        sides.append((ev, tail))
    return sides


def kernel(
    experts,
    tok_ref, gain_ref, ids_ref, mix_ref, wg_hbm, wu_hbm, wd_hbm,
    out_ref,
    wg, wu, wd, normed, disp, xin, hid, part, r1, r2s, r2r, r3s, home, acc,
    w_sem, zs_sem, zr_sem, ys_sem, yr_sem, cs_sem, cr_sem, ds_sem, dr_sem,
    r1s_sem, r1r_sem, r2s_sem, r2r_sem, r3s_sem, r3r_sem,
):
    me = lax.axis_index("ep")
    z = me // SPLIT
    y = (me // 2) % 2
    c = me % 2
    rows, width = tok_ref.shape
    cap = disp.shape[1]
    nq = cap // CHUNK
    ff = wg.shape[1]
    top = ids_ref.shape[0]
    at_y = {"ep": z * SPLIT + (1 - y) * 2 + c}
    at_c = {"ep": z * SPLIT + y * 2 + (1 - c)}
    mine = c * 2 + y
    other_y = c * 2 + 1 - y
    other_c = (1 - c) * 2 + y
    other_yc = (1 - c) * 2 + 1 - y
    near = jnp.minimum(z, experts - 1 - z)
    away = jnp.where(2 * z < experts, 1, -1)
    inner = near > 0
    edge = near == 0

    def peer(k):
        both = z + away * ((k + 1) // 2) * (2 * (k % 2) - 1)
        from_edge = z + away * jnp.where(k < 2, k, experts + 1 - k)
        from_inner = jnp.where(k <= 2 * near, both, z + away * (k - near))
        return jnp.where(edge, from_edge, from_inner)

    def at_z(k):
        return {"ep": peer(k) * SPLIT + y * 2 + c}

    def remote(src, dst, send, recv, where):
        return pltpu.make_async_remote_copy(
            src_ref=src, dst_ref=dst, send_sem=send, recv_sem=recv,
            device_id=where, device_id_type=pl.DeviceIdType.MESH,
        )

    def chunk(q):
        return pl.ds(pl.multiple_of(q * CHUNK, CHUNK), CHUNK)

    ff_cuts = cut(ff, 3)
    out_cuts = cut(width, 2)
    pieces = w_sem.shape[1]

    def weight(which):
        hbm, vmem = ((wg_hbm, wg), (wu_hbm, wu), (wd_hbm, wd))[which]
        size = hbm.shape[0] // pieces
        return [
            pltpu.make_async_copy(
                hbm.at[pl.ds(i * size, size)], vmem.at[pl.ds(i * size, size)], w_sem.at[which, i]
            )
            for i in range(pieces)
        ]

    barrier = pltpu.get_barrier_semaphore()
    for k in range(1, experts):
        pl.semaphore_signal(barrier, inc=1, device_id=at_z(k), device_id_type=pl.DeviceIdType.MESH)
    pl.semaphore_signal(barrier, inc=1, device_id=at_y, device_id_type=pl.DeviceIdType.MESH)
    pl.semaphore_signal(barrier, inc=1, device_id=at_c, device_id_type=pl.DeviceIdType.MESH)

    for which in range(3):
        for copy in weight(which):
            copy.start()

    step = tile_of(rows, 32)

    @pl.loop(0, rows // step)
    def _(r):
        at = pl.ds(pl.multiple_of(r * step, step), step)
        values = tok_ref[at, :].astype(f32)
        scale = lax.rsqrt(jnp.mean(values * values, axis=-1, keepdims=True) + 1e-06)
        normed[at, :] = (values * scale * gain_ref[...]).astype(bf16)

    lanes = 128
    expert_row = lax.broadcasted_iota(jnp.int32, (lanes, rows), 0)
    named = ids_ref[0:1, :] == expert_row
    weight_t = jnp.where(named, mix_ref[0:1, :], 0.0)
    for k in range(1, top):
        hit = ids_ref[k : k + 1, :] == expert_row
        named = named | hit
        weight_t = weight_t + jnp.where(hit, mix_ref[k : k + 1, :], 0.0)
    named = named.astype(f32)
    first = lax.broadcasted_iota(jnp.int32, (rows, rows), 0)
    second = lax.broadcasted_iota(jnp.int32, (rows, rows), 1)
    upper = (first < second).astype(f32).astype(bf16)
    rank_t = jnp.dot(named.astype(bf16), upper, preferred_element_type=f32)
    rank_t = jnp.where(named > 0.5, rank_t, -1.0)
    rank = jnp.transpose(rank_t)
    weight_c = jnp.transpose(weight_t)
    lane = lax.broadcasted_iota(jnp.int32, (rows, lanes), 1)

    def dispatch(e, dst):
        slot = jnp.sum(jnp.where(expert_row == e, rank_t, 0.0), axis=0, keepdims=True)
        place = lax.broadcasted_iota(jnp.int32, (cap, rows), 0)
        pick = (place == slot.astype(jnp.int32)).astype(f32).astype(bf16)
        wide = tile_of(width, 512)
        for n in range(width // wide):
            cols = slice(n * wide, (n + 1) * wide)
            dst[:, cols] = jnp.dot(pick, normed[:, cols], preferred_element_type=f32).astype(bf16)

    def z_copy(k, q):
        return remote(disp.at[k, chunk(q)], xin.at[z, mine, chunk(q)], zs_sem.at[k, q], zr_sem.at[z, q], at_z(k))

    def z_arrival(k, q):
        p = peer(k)
        return remote(disp.at[k, chunk(q)], xin.at[p, mine, chunk(q)], zs_sem.at[k, q], zr_sem.at[p, q], at_z(k))

    def send_z(k):
        @pl.loop(0, nq)
        def _(q):
            z_copy(k, q).start()

    def in_group(sub, send, recv, where):
        def make(k, q):
            slot = xin.at[peer(k), sub, chunk(q)]
            return remote(slot, slot, send.at[k, q], recv.at[k, q], where)

        return make

    y_copy = in_group(mine, ys_sem, yr_sem, at_y)
    y_arrival = in_group(other_y, ys_sem, yr_sem, at_y)
    c_copy = in_group(mine, cs_sem, cr_sem, at_c)
    c_arrival = in_group(other_c, cs_sem, cr_sem, at_c)
    d_copy = in_group(other_y, ds_sem, dr_sem, at_c)
    d_arrival = in_group(other_yc, ds_sem, dr_sem, at_c)

    def r1_copy(k, v, h):
        start, size = out_cuts[h]
        cols = pl.ds(start, size)
        return remote(
            part.at[k, 1 - c, v, :, cols], r1.at[k, v, :, cols], r1s_sem.at[k, v, h], r1r_sem.at[k, v, h], at_c
        )

    def r2_copy(k, q):
        return remote(r2s.at[k, chunk(q)], r2r.at[k, chunk(q)], r2s_sem.at[k, q], r2r_sem.at[k, q], at_y)

    def r3_copy(k, q):
        return remote(r3s.at[k, chunk(q)], home.at[z, chunk(q)], r3s_sem.at[k, q], r3r_sem.at[z, q], at_z(k))

    def r3_arrival(k, q):
        p = peer(k)
        return remote(r3s.at[k, chunk(q)], home.at[p, chunk(q)], r3s_sem.at[k, q], r3r_sem.at[p, q], at_z(k))

    def forward_z(k, q):
        if k > 0:
            z_arrival(k, q).wait_recv()
        y_copy(k, q).start()
        c_copy(k, q).start()

    def forward_y(k, q):
        y_arrival(k, q).wait_recv()
        d_copy(k, q).start()

    def chip_sum(k, q):
        at = chunk(q)

        @pl.when(q == 0)
        def _():
            for h in range(2):
                r1_copy(k, 1 - y, h).wait_recv()

        r2s[k, at, :] = (part[k, c, 1 - y, at, :].astype(f32) + r1[k, 1 - y, at, :].astype(f32)).astype(bf16)
        r2_copy(k, q).start()

    def group_sum(k, q):
        at = chunk(q)

        @pl.when(q == 0)
        def _():
            for h in range(2):
                r1_copy(k, y, h).wait_recv()

        r2_copy(k, q).wait_recv()
        total = (
            part[k, c, y, at, :].astype(f32) + r1[k, y, at, :].astype(f32) + r2r[k, at, :].astype(f32)
        ).astype(bf16)
        if k == 0:
            home[z, at, :] = total
        else:
            r3s[k, at, :] = total
            r3_copy(k, q).start()

    def mix(k):
        e = peer(k)
        if k > 0:
            @pl.loop(0, nq)
            def _(q):
                r3_arrival(k, q).wait_recv()

        slot = jnp.sum(jnp.where(lane == e, rank, 0.0), axis=1, keepdims=True)
        share = jnp.sum(jnp.where(lane == e, weight_c, 0.0), axis=1, keepdims=True)
        place = lax.broadcasted_iota(jnp.int32, (rows, cap), 1)
        pick = (place == slot.astype(jnp.int32)).astype(f32).astype(bf16)
        wide = tile_of(width, 512)
        for n in range(width // wide):
            cols = slice(n * wide, (n + 1) * wide)
            acc[:, cols] += share * jnp.dot(pick, home[e, :, cols], preferred_element_type=f32)

    actions = {"z": forward_z, "y": forward_y, "chip": chip_sum, "group": group_sum}
    sides = plan(experts, nq)

    def perform(items):
        for item in items:
            if item[0] == "mix":
                mix(item[1])
            else:
                kind, k, lo, hi = item

                @pl.loop(lo, hi)
                def _(q):
                    actions[kind](k, q)

    def service(step_index, place):
        for k in range(experts):
            lists = [side[0].get((k, place), []) for side in sides]
            if lists[0] == lists[1]:
                if lists[0]:
                    @pl.when(step_index == k)
                    def _():
                        perform(lists[0])
            else:
                for items, kind in zip(lists, (edge, inner)):
                    if items:
                        @pl.when((step_index == k) & kind)
                        def _():
                            perform(items)

    dispatch(z, xin.at[z, mine])
    pl.semaphore_wait(barrier, experts + 1)

    @pl.loop(0, nq)
    def _(q):
        forward_z(0, q)

    @pl.loop(1, experts)
    def _(k):
        dispatch(peer(k), disp.at[k])

        @pl.when((k == 1) | (inner & (k == 2)))
        def _():
            send_z(k)

    acc[...] = jnp.zeros_like(acc)

    @pl.loop(0, nq)
    def _(q):
        forward_y(0, q)
        if experts > 1:
            forward_z(1, q)

    @pl.loop(2, experts)
    def _(k):
        @pl.when(edge | (k > 2))
        def _():
            send_z(k)

    for which in range(3):
        for copy in weight(which):
            copy.wait()

    @pl.loop(0, experts)
    def _(k):
        @pl.loop(0, nq)
        def _(q):
            c_arrival(k, q).wait_recv()
            d_arrival(k, q).wait_recv()

        for h, (start, size) in enumerate(ff_cuts):
            cols = slice(start, start + size)
            inputs = xin[peer(k)].reshape(SPLIT * cap, width)
            gate = jnp.dot(inputs, wg[:, cols], preferred_element_type=f32)
            up = jnp.dot(inputs, wu[:, cols], preferred_element_type=f32)
            hid[:, cols] = (gate / (1.0 + jnp.exp(-gate)) * up).astype(bf16)
            service(k, 1 + h)

        for h, (start, size) in enumerate(out_cuts):
            cols = slice(start, start + size)
            res = jnp.dot(hid[...], wd[:, cols], preferred_element_type=f32).astype(bf16)
            part[k, :, :, :, cols] = res.reshape(2, 2, cap, size)
            for v in (1 - y, y):
                r1_copy(k, v, h).start()
            service(k, 1 + len(ff_cuts) + h)

    tails = [side[1] for side in sides]
    if tails[0] == tails[1]:
        perform(tails[0])
    else:
        for items, kind in zip(tails, (edge, inner)):
            @pl.when(kind)
            def _():
                perform(items)

    out_ref[...] = acc[...].astype(bf16)

    @pl.loop(0, experts)
    def _(k):
        @pl.when(k > 0)
        def _():
            @pl.loop(0, nq)
            def _(q):
                z_copy(k, q).wait_send()
                r3_copy(k, q).wait_send()

        @pl.loop(0, nq)
        def _(q):
            y_copy(k, q).wait_send()
            c_copy(k, q).wait_send()
            d_copy(k, q).wait_send()
            r2_copy(k, q).wait_send()

        for v in range(2):
            for h in range(2):
                r1_copy(k, v, h).wait_send()


def local(tokens, norm_gain, expert_ids, mix_weights, gate_weight, up_weight, down_weight):
    n_dev = lax.axis_size("ep")
    experts = n_dev // SPLIT
    rows, width = tokens.shape
    top = expert_ids.shape[1]
    ff = gate_weight.shape[1]
    cap = (rows * top * SPLIT * 5 + 4 * n_dev - 1) // (4 * n_dev)
    cap = (cap + CHUNK - 1) // CHUNK * CHUNK
    nq = cap // CHUNK
    dma = pltpu.SemaphoreType.DMA
    vmem = pl.BlockSpec(memory_space=pltpu.VMEM)
    hbm = pl.BlockSpec(memory_space=pl.ANY)
    block = (cap, width)
    return pl.pallas_call(
        functools.partial(kernel, experts),
        out_shape=jax.ShapeDtypeStruct((rows, width), bf16),
        in_specs=[vmem, vmem, vmem, vmem, hbm, hbm, hbm],
        out_specs=vmem,
        scratch_shapes=[
            pltpu.VMEM((width, ff), bf16),
            pltpu.VMEM((width, ff), bf16),
            pltpu.VMEM((ff, width), bf16),
            pltpu.VMEM((rows, width), bf16),
            pltpu.VMEM((experts,) + block, bf16),
            pltpu.VMEM((experts, SPLIT) + block, bf16),
            pltpu.VMEM((SPLIT * cap, ff), bf16),
            pltpu.VMEM((experts, 2, 2) + block, bf16),
            pltpu.VMEM((experts, 2) + block, bf16),
            pltpu.VMEM((experts,) + block, bf16),
            pltpu.VMEM((experts,) + block, bf16),
            pltpu.VMEM((experts,) + block, bf16),
            pltpu.VMEM((experts,) + block, bf16),
            pltpu.VMEM((rows, width), f32),
            dma((3, 4)),
        ] + [dma((experts, nq))] * 8 + [dma((experts, 2, 2))] * 2 + [dma((experts, nq))] * 4,
        compiler_params=pltpu.CompilerParams(
            collective_id=0, has_side_effects=True, vmem_limit_bytes=64 * 1024 * 1024 - 65536,
        ),
    )(tokens, norm_gain.reshape(1, width), expert_ids.T, mix_weights.T, gate_weight, up_weight, down_weight)


def solution(mesh):
    in_specs = (
        P(("grp", "ep"), None),
        P(),
        P(("grp", "ep"), None),
        P(("grp", "ep"), None),
        P(None, "ep"),
        P(None, "ep"),
        P("ep", None),
    )
    out_specs = P(("grp", "ep"), None)
    return jax.shard_map(local, mesh=mesh, in_specs=in_specs, out_specs=out_specs, check_vma=False)
```

```python
import functools

import jax
import jax.numpy as jnp
from jax import lax
from jax.experimental import pallas as pl
from jax.experimental.pallas import tpu as pltpu
from jax.sharding import PartitionSpec as P

SPLIT = 4
CHUNK = 16
f32, bf16 = jnp.float32, jnp.bfloat16


def tile_of(extent, most):
    tile = most
    while extent % tile:
        tile //= 2
    return tile


def cut(extent, parts):
    tiles = extent // 256
    ends = [tiles * i // parts * 256 for i in range(parts)] + [extent]
    return tuple((a, b - a) for a, b in zip(ends, ends[1:]))


def plan(experts, nq):
    last = experts - 1
    sides = []
    for inner in (False, True):
        ev = {}

        def at(step, place, *items, ev=ev):
            ev.setdefault((step, place), []).extend(
                (kind, k, nq * lo // 5, nq * hi // 5) for kind, k, lo, hi in items
            )

        if experts == 4:
            if inner:
                at(0, 1, ("z", 3, 0, 2))
                at(0, 3, ("y", 1, 0, 4))
                at(0, 4, ("y", 1, 4, 5), ("z", 3, 2, 4))
                at(1, 1, ("z", 2, 0, 1))
                at(1, 2, ("z", 2, 1, 3))
                at(1, 3, ("z", 2, 3, 4))
                at(1, 4, ("z", 2, 4, 5))
                at(1, 5, ("chip", 1, 0, 5), ("y", 2, 0, 3), ("z", 3, 4, 5), ("chip", 1, 5, 10))
                at(1, 5, ("y", 2, 3, 5))
                at(2, 1, ("group", 1, 0, 1))
                at(2, 2, ("group", 1, 1, 4))
                at(2, 3, ("chip", 0, 0, 3), ("group", 1, 4, 7))
                at(2, 4, ("y", 3, 0, 5), ("group", 1, 7, 8))
                at(2, 5, ("chip", 2, 0, 5), ("group", 1, 8, 10), ("chip", 2, 5, 10))
                at(3, 1, ("group", 2, 0, 1))
                at(3, 2, ("group", 2, 1, 4))
                at(3, 3, ("group", 2, 4, 7))
                at(3, 4, ("chip", 0, 3, 5), ("group", 2, 7, 9))
                at(3, 5, ("chip", 3, 0, 5), ("group", 2, 9, 10))
                at(4, 0, ("chip", 3, 5, 10), ("chip", 0, 5, 10), ("group", 0, 0, 5))
                at(4, 0, ("mix", 1, 0, 5), ("group", 3, 0, 10), ("group", 0, 5, 10))
                at(4, 0, ("mix", 0, 0, 5), ("mix", 3, 0, 5), ("mix", 2, 0, 5))
            else:
                at(0, 2, ("z", 2, 0, 1))
                at(0, 3, ("z", 2, 1, 2), ("y", 1, 0, 4))
                at(0, 4, ("y", 1, 4, 5), ("z", 2, 2, 4))
                at(0, 5, ("z", 2, 4, 5))
                at(1, 1, ("chip", 0, 0, 4))
                at(1, 3, ("chip", 0, 4, 6), ("y", 2, 0, 5))
                at(1, 4, ("z", 3, 0, 1))
                at(1, 5, ("z", 3, 1, 2))
                at(2, 1, ("z", 3, 2, 4))
                at(2, 2, ("z", 3, 4, 5))
                at(2, 3, ("chip", 1, 0, 2), ("y", 3, 0, 2))
                at(2, 4, ("chip", 1, 2, 4), ("y", 3, 2, 5))
                at(2, 5, ("chip", 2, 0, 10))
                at(3, 1, ("group", 1, 0, 4))
                at(3, 2, ("group", 2, 0, 2))
                at(3, 3, ("group", 2, 2, 5))
                at(3, 4, ("chip", 1, 4, 7), ("group", 2, 5, 8))
                at(3, 5, ("chip", 3, 0, 5), ("group", 2, 8, 9))
                at(4, 0, ("chip", 3, 5, 10), ("chip", 1, 7, 10), ("chip", 0, 6, 10), ("group", 2, 9, 10))
                at(4, 0, ("group", 1, 4, 7), ("group", 0, 0, 6), ("group", 3, 0, 10), ("mix", 2, 0, 5))
                at(4, 0, ("group", 1, 7, 10), ("group", 0, 6, 10))
                at(4, 0, ("mix", 0, 0, 5), ("mix", 3, 0, 5), ("mix", 1, 0, 5))
        else:
            for k in range(experts):
                if k + 2 < experts:
                    at(k, 2, ("z", k + 2, 0, 5))
                if k + 1 < experts:
                    at(k, 5, ("y", k + 1, 0, 5))
                if k > 0:
                    at(k, 1, ("chip", k - 1, 0, 10))
                    at(k, 3, ("group", k - 1, 0, 10))
            at(experts, 0, ("chip", last, 0, 10), ("group", last, 0, 10))
            at(experts, 0, *[("mix", k, 0, 5) for k in range(experts)])
        tail = ev.pop((experts, 0))
        sides.append((ev, tail))
    return sides


def kernel(
    experts,
    tok_ref, gain_ref, ids_ref, mix_ref, wg_hbm, wu_hbm, wd_hbm,
    out_ref,
    wg, wu, wd, normed, disp, xin, hid, part, r1, r2s, r2r, r3s, home, acc,
    w_sem, zs_sem, zr_sem, ys_sem, yr_sem, cs_sem, cr_sem, ds_sem, dr_sem,
    r1s_sem, r1r_sem, r2s_sem, r2r_sem, r3s_sem, r3r_sem,
):
    me = lax.axis_index("ep")
    z = me // SPLIT
    y = (me // 2) % 2
    c = me % 2
    rows, width = tok_ref.shape
    cap = disp.shape[1]
    nq = cap // CHUNK
    ff = wg.shape[1]
    top = ids_ref.shape[0]
    at_y = {"ep": z * SPLIT + (1 - y) * 2 + c}
    at_c = {"ep": z * SPLIT + y * 2 + (1 - c)}
    mine = c * 2 + y
    other_y = c * 2 + 1 - y
    other_c = (1 - c) * 2 + y
    other_yc = (1 - c) * 2 + 1 - y
    near = jnp.minimum(z, experts - 1 - z)
    away = jnp.where(2 * z < experts, 1, -1)
    inner = near > 0
    edge = near == 0

    def peer(k):
        from_edge = z + away * jnp.where(k < 2, k, experts + 1 - k)
        n = jnp.where(k < 2, k, jnp.where(k == experts - 1, 2, k + 1))
        both = z + away * ((n + 1) // 2) * (2 * (n % 2) - 1)
        from_inner = jnp.where(n <= 2 * near, both, z + away * (n - near))
        return jnp.where(edge, from_edge, from_inner)

    def at_z(k):
        return {"ep": peer(k) * SPLIT + y * 2 + c}

    def remote(src, dst, send, recv, where):
        return pltpu.make_async_remote_copy(
            src_ref=src, dst_ref=dst, send_sem=send, recv_sem=recv,
            device_id=where, device_id_type=pl.DeviceIdType.MESH,
        )

    def chunk(q):
        return pl.ds(pl.multiple_of(q * CHUNK, CHUNK), CHUNK)

    ff_cuts = cut(ff, 3)
    out_cuts = cut(width, 2)
    pieces = 4

    def weight(which):
        hbm, vmem = ((wg_hbm, wg), (wu_hbm, wu), (wd_hbm, wd))[which]
        size = hbm.shape[0] // pieces
        return [
            pltpu.make_async_copy(
                hbm.at[pl.ds(i * size, size)], vmem.at[pl.ds(i * size, size)], w_sem.at[which]
            )
            for i in range(pieces)
        ]

    barrier = pltpu.get_barrier_semaphore()
    for k in range(1, experts):
        pl.semaphore_signal(barrier, inc=1, device_id=at_z(k), device_id_type=pl.DeviceIdType.MESH)
    pl.semaphore_signal(barrier, inc=1, device_id=at_y, device_id_type=pl.DeviceIdType.MESH)
    pl.semaphore_signal(barrier, inc=1, device_id=at_c, device_id_type=pl.DeviceIdType.MESH)

    for which in range(3):
        for copy in weight(which):
            copy.start()

    step = tile_of(rows, 32)

    @pl.loop(0, rows // step)
    def _(r):
        at = pl.ds(pl.multiple_of(r * step, step), step)
        values = tok_ref[at, :].astype(f32)
        scale = lax.rsqrt(jnp.mean(values * values, axis=-1, keepdims=True) + 1e-06)
        normed[at, :] = (values * scale * gain_ref[...]).astype(bf16)

    lanes = 128
    expert_row = lax.broadcasted_iota(jnp.int32, (lanes, rows), 0)
    named = ids_ref[0:1, :] == expert_row
    weight_t = jnp.where(named, mix_ref[0:1, :], 0.0)
    for k in range(1, top):
        hit = ids_ref[k : k + 1, :] == expert_row
        named = named | hit
        weight_t = weight_t + jnp.where(hit, mix_ref[k : k + 1, :], 0.0)
    named = named.astype(f32)
    first = lax.broadcasted_iota(jnp.int32, (rows, rows), 0)
    second = lax.broadcasted_iota(jnp.int32, (rows, rows), 1)
    upper = (first < second).astype(f32).astype(bf16)
    rank_t = jnp.dot(named.astype(bf16), upper, preferred_element_type=f32)
    rank_t = jnp.where(named > 0.5, rank_t, -1.0)
    rank = jnp.transpose(rank_t)
    weight_c = jnp.transpose(weight_t)
    lane = lax.broadcasted_iota(jnp.int32, (rows, lanes), 1)

    def dispatch(e, dst):
        slot = jnp.sum(jnp.where(expert_row == e, rank_t, 0.0), axis=0, keepdims=True)
        place = lax.broadcasted_iota(jnp.int32, (cap, rows), 0)
        pick = (place == slot.astype(jnp.int32)).astype(f32).astype(bf16)
        wide = tile_of(width, 512)
        for n in range(width // wide):
            cols = slice(n * wide, (n + 1) * wide)
            dst[:, cols] = jnp.dot(pick, normed[:, cols], preferred_element_type=f32).astype(bf16)

    def z_copy(k, q):
        return remote(disp.at[k, chunk(q)], xin.at[z, mine, chunk(q)], zs_sem, zr_sem.at[z, q], at_z(k))

    def z_arrival(k, q):
        p = peer(k)
        return remote(disp.at[k, chunk(q)], xin.at[p, mine, chunk(q)], zs_sem, zr_sem.at[p, q], at_z(k))

    def send_z(k):
        @pl.loop(0, nq)
        def _(q):
            z_copy(k, q).start()

    def in_group(sub, send, recv, where):
        def make(k, q):
            slot = xin.at[peer(k), sub, chunk(q)]
            return remote(slot, slot, send, recv(k, q), where)

        return make

    y_copy = in_group(mine, ys_sem, lambda k, q: yr_sem.at[k, q], at_y)
    y_arrival = in_group(other_y, ys_sem, lambda k, q: yr_sem.at[k, q], at_y)
    c_copy = in_group(mine, cs_sem, lambda k, q: cr_sem.at[k], at_c)
    d_copy = in_group(other_y, ds_sem, lambda k, q: dr_sem.at[k], at_c)

    def c_arrival(k):
        slot = xin.at[peer(k), other_c]
        return remote(slot, slot, cs_sem, cr_sem.at[k], at_c)

    def d_arrival(k):
        slot = xin.at[peer(k), other_yc]
        return remote(slot, slot, ds_sem, dr_sem.at[k], at_c)

    def r1_copy(k, v, h):
        start, size = out_cuts[h]
        cols = pl.ds(start, size)
        return remote(
            part.at[k, 1 - c, v, :, cols], r1.at[k, v, :, cols], r1s_sem, r1r_sem.at[k, v, h], at_c
        )

    def piece(u):
        cols = pl.ds(pl.multiple_of(u // nq * (width // 2), width // 2), width // 2)
        return chunk(u % nq), cols

    def r2_copy(k, u):
        at = (k,) + piece(u)
        return remote(r2s.at[at], r2r.at[at], r2s_sem, r2r_sem.at[k, u], at_y)

    def r3_copy(k, u):
        at = piece(u)
        return remote(r3s.at[(k,) + at], home.at[(z,) + at], r3s_sem, r3r_sem.at[z], at_z(k))

    def r3_arrival(k):
        p = peer(k)
        return remote(r3s.at[k], home.at[p], r3s_sem, r3r_sem.at[p], at_z(k))

    def forward_z(k, q):
        if k > 0:
            z_arrival(k, q).wait_recv()
        y_copy(k, q).start()
        c_copy(k, q).start()

    def forward_y(k, q):
        y_arrival(k, q).wait_recv()
        d_copy(k, q).start()

    def r1_wait(k, v, u):
        for h in range(2):
            @pl.when(u == h * nq)
            def _():
                r1_copy(k, v, h).wait_recv()

    def chip_sum(k, u):
        at, cols = piece(u)
        r1_wait(k, 1 - y, u)
        r2s[k, at, cols] = (
            part[k, c, 1 - y, at, cols].astype(f32) + r1[k, 1 - y, at, cols].astype(f32)
        ).astype(bf16)
        r2_copy(k, u).start()

    def group_sum(k, u):
        at, cols = piece(u)
        r1_wait(k, y, u)
        r2_copy(k, u).wait_recv()
        total = (
            part[k, c, y, at, cols].astype(f32) + r1[k, y, at, cols].astype(f32) + r2r[k, at, cols].astype(f32)
        ).astype(bf16)
        if k == 0:
            home[z, at, cols] = total
        else:
            r3s[k, at, cols] = total
            r3_copy(k, u).start()

    def mix(k):
        e = peer(k)
        if k > 0:
            r3_arrival(k).wait_recv()

        slot = jnp.sum(jnp.where(lane == e, rank, 0.0), axis=1, keepdims=True)
        share = jnp.sum(jnp.where(lane == e, weight_c, 0.0), axis=1, keepdims=True)
        place = lax.broadcasted_iota(jnp.int32, (rows, cap), 1)
        pick = (place == slot.astype(jnp.int32)).astype(f32).astype(bf16)
        wide = tile_of(width, 512)
        for n in range(width // wide):
            cols = slice(n * wide, (n + 1) * wide)
            acc[:, cols] += share * jnp.dot(pick, home[e, :, cols], preferred_element_type=f32)

    actions = {"z": forward_z, "y": forward_y, "chip": chip_sum, "group": group_sum}
    sides = plan(experts, nq)

    def perform(items):
        for item in items:
            if item[0] == "mix":
                mix(item[1])
            else:
                kind, k, lo, hi = item

                @pl.loop(lo, hi)
                def _(q):
                    actions[kind](k, q)

    def service(step_index, place):
        for k in range(experts):
            lists = [side[0].get((k, place), []) for side in sides]
            if lists[0] == lists[1]:
                if lists[0]:
                    @pl.when(step_index == k)
                    def _():
                        perform(lists[0])
            else:
                for items, kind in zip(lists, (edge, inner)):
                    if items:
                        @pl.when((step_index == k) & kind)
                        def _():
                            perform(items)

    dispatch(z, xin.at[z, mine])
    pl.semaphore_wait(barrier, experts + 1)

    @pl.loop(0, nq)
    def _(q):
        forward_z(0, q)

    @pl.loop(1, experts)
    def _(k):
        dispatch(peer(k), disp.at[k])

        @pl.when((k == 1) | (inner & (k == experts - 1)))
        def _():
            send_z(k)

    acc[...] = jnp.zeros_like(acc)

    lead = min(2, nq)

    @pl.loop(0, lead)
    def _(q):
        forward_y(0, q)

    @pl.loop(lead, nq)
    def _(q):
        forward_z(1, q - lead)
        forward_y(0, q)

    @pl.loop(nq - lead, nq)
    def _(q):
        forward_z(1, q)

    @pl.loop(2, experts)
    def _(k):
        @pl.when(edge | (k < experts - 1))
        def _():
            send_z(k)

    for which, (hbm, vmem) in enumerate(((wg_hbm, wg), (wu_hbm, wu), (wd_hbm, wd))):
        pltpu.make_async_copy(hbm, vmem, w_sem.at[which]).wait()

    @pl.loop(0, experts)
    def _(k):
        c_arrival(k).wait_recv()
        d_arrival(k).wait_recv()

        for h, (start, size) in enumerate(ff_cuts):
            cols = slice(start, start + size)
            inputs = xin[peer(k)].reshape(SPLIT * cap, width)
            gate = jnp.dot(inputs, wg[:, cols], preferred_element_type=f32)
            up = jnp.dot(inputs, wu[:, cols], preferred_element_type=f32)
            hid[:, cols] = (gate / (1.0 + jnp.exp(-gate)) * up).astype(bf16)
            service(k, 1 + h)

        for h, (start, size) in enumerate(out_cuts):
            cols = slice(start, start + size)
            res = jnp.dot(hid[...], wd[:, cols], preferred_element_type=f32).astype(bf16)
            part[k, :, :, :, cols] = res.reshape(2, 2, cap, size)
            for v in (1 - y, y):
                r1_copy(k, v, h).start()
            service(k, 1 + len(ff_cuts) + h)

    tails = [side[1] for side in sides]
    if tails[0] == tails[1]:
        perform(tails[0])
    else:
        for items, kind in zip(tails, (edge, inner)):
            @pl.when(kind)
            def _():
                perform(items)

    out_ref[...] = acc[...].astype(bf16)

    others = pl.ds(1, experts - 1)
    remote(disp.at[others], disp.at[others], zs_sem, cr_sem.at[0], at_c).wait_send()
    remote(disp, disp, ys_sem, cr_sem.at[0], at_c).wait_send()
    remote(disp, disp, cs_sem, cr_sem.at[0], at_c).wait_send()
    remote(disp, disp, ds_sem, cr_sem.at[0], at_c).wait_send()
    remote(part.at[:, 0], r1, r1s_sem, cr_sem.at[0], at_c).wait_send()
    remote(r2s, r2r, r2s_sem, cr_sem.at[0], at_c).wait_send()
    remote(r3s.at[others], home.at[others], r3s_sem, cr_sem.at[0], at_c).wait_send()


def local(tokens, norm_gain, expert_ids, mix_weights, gate_weight, up_weight, down_weight):
    n_dev = lax.axis_size("ep")
    experts = n_dev // SPLIT
    rows, width = tokens.shape
    top = expert_ids.shape[1]
    ff = gate_weight.shape[1]
    cap = (rows * top * SPLIT * 5 + 4 * n_dev - 1) // (4 * n_dev)
    cap = (cap + CHUNK - 1) // CHUNK * CHUNK
    nq = cap // CHUNK
    dma = pltpu.SemaphoreType.DMA
    vmem = pl.BlockSpec(memory_space=pltpu.VMEM)
    hbm = pl.BlockSpec(memory_space=pl.ANY)
    block = (cap, width)
    return pl.pallas_call(
        functools.partial(kernel, experts),
        out_shape=pltpu.VMEM((rows, width), bf16),
        in_specs=[vmem, vmem, vmem, vmem, hbm, hbm, hbm],
        out_specs=vmem,
        scratch_shapes=[
            pltpu.VMEM((width, ff), bf16),
            pltpu.VMEM((width, ff), bf16),
            pltpu.VMEM((ff, width), bf16),
            pltpu.VMEM((rows, width), bf16),
            pltpu.VMEM((experts,) + block, bf16),
            pltpu.VMEM((experts, SPLIT) + block, bf16),
            pltpu.VMEM((SPLIT * cap, ff), bf16),
            pltpu.VMEM((experts, 2, 2) + block, bf16),
            pltpu.VMEM((experts, 2) + block, bf16),
            pltpu.VMEM((experts,) + block, bf16),
            pltpu.VMEM((experts,) + block, bf16),
            pltpu.VMEM((experts,) + block, bf16),
            pltpu.VMEM((experts,) + block, bf16),
            pltpu.VMEM((rows, width), f32),
            dma((3,)),
                    dma, dma((experts, nq)), dma, dma((experts, nq)), dma, dma((experts,)), dma, dma((experts,)),
            dma, dma((experts, 2, 2)), dma, dma((experts, 2 * nq)), dma, dma((experts,)),
        ],
        compiler_params=pltpu.CompilerParams(
            collective_id=0, has_side_effects=True, vmem_limit_bytes=58 * 1024 * 1024,
        ),
    )(tokens, norm_gain.reshape(1, width), expert_ids.T, mix_weights.T, gate_weight, up_weight, down_weight)


def solution(mesh):
    in_specs = (
        P(("grp", "ep"), None),
        P(),
        P(("grp", "ep"), None),
        P(("grp", "ep"), None),
        P(None, "ep"),
        P(None, "ep"),
        P("ep", None),
    )
    out_specs = P(("grp", "ep"), None)
    return jax.shard_map(local, mesh=mesh, in_specs=in_specs, out_specs=out_specs, check_vma=False)
```

```python
import functools

import jax
import jax.numpy as jnp
from jax import lax
from jax.experimental import pallas as pl
from jax.experimental.pallas import tpu as pltpu
from jax.sharding import PartitionSpec as P

SPLIT = 4
CHUNK = 16
f32, bf16 = jnp.float32, jnp.bfloat16


def tile_of(extent, most):
    tile = most
    while extent % tile:
        tile //= 2
    return tile


def cut(extent, parts):
    tiles = extent // 256
    ends = [tiles * i // parts * 256 for i in range(parts)] + [extent]
    return tuple((a, b - a) for a, b in zip(ends, ends[1:]))


def plan(experts, nq):
    last = experts - 1
    sides = []
    for inner in (False, True):
        ev = {}

        def at(step, place, *items, ev=ev):
            ev.setdefault((step, place), []).extend(
                item if item[0] == "end" else (item[0], item[1], nq * item[2] // 5, nq * item[3] // 5)
                for item in items
            )

        if experts == 4:
            if inner:
                at(0, 1, ("z", 3, 0, 2))
                at(0, 3, ("y", 1, 0, 4))
                at(0, 4, ("y", 1, 4, 5), ("z", 3, 2, 4))
                at(1, 1, ("z", 2, 0, 1))
                at(1, 2, ("z", 2, 1, 3))
                at(1, 3, ("z", 2, 3, 4))
                at(1, 4, ("z", 2, 4, 5))
                at(1, 5, ("chip", 1, 0, 5), ("y", 2, 0, 3), ("z", 3, 4, 5), ("chip", 1, 5, 10))
                at(1, 5, ("y", 2, 3, 5))
                at(2, 1, ("group", 1, 0, 1))
                at(2, 2, ("group", 1, 1, 4))
                at(2, 3, ("chip", 0, 0, 3), ("group", 1, 4, 7))
                at(2, 4, ("y", 3, 0, 5), ("group", 1, 7, 8))
                at(2, 5, ("chip", 2, 0, 5), ("group", 1, 8, 10), ("chip", 2, 5, 10))
                at(3, 1, ("group", 2, 0, 1))
                at(3, 2, ("group", 2, 1, 4))
                at(3, 3, ("chip", 0, 3, 6), ("group", 2, 4, 7))
                at(3, 4, ("group", 2, 7, 9))
                at(3, 5, ("chip", 3, 0, 5), ("group", 2, 9, 10))
                at(4, 0, ("chip", 3, 5, 10), ("group", 0, 0, 6))
                at(4, 0, ("mix", 1, 0, 5), ("group", 3, 0, 6), ("chip", 0, 6, 10), ("group", 3, 6, 10))
                at(4, 0, ("group", 0, 6, 10), ("mix", 0, 0, 5), ("end", 3, 2))
            else:
                at(0, 2, ("z", 1, 0, 1))
                at(0, 3, ("z", 1, 1, 2), ("y", 2, 0, 4))
                at(0, 4, ("y", 2, 4, 5), ("z", 1, 2, 4))
                at(0, 5, ("z", 1, 4, 5), ("y", 1, 0, 3), ("chip", 0, 0, 4), ("y", 1, 3, 5))
                at(1, 1, ("chip", 0, 4, 6))
                at(1, 2, ("z", 3, 0, 1))
                at(1, 3, ("z", 3, 1, 2))
                at(1, 4, ("z", 3, 2, 4))
                at(1, 5, ("z", 3, 4, 5), ("chip", 1, 0, 10))
                at(2, 2, ("y", 3, 0, 5))
                at(2, 3, ("group", 1, 0, 3))
                at(2, 4, ("group", 1, 3, 5))
                at(2, 5, ("chip", 2, 0, 5), ("group", 1, 5, 7))
                at(3, 1, ("chip", 2, 5, 10), ("group", 1, 7, 9))
                at(3, 2, ("group", 1, 9, 10))
                at(3, 3, ("group", 2, 0, 3))
                at(3, 4, ("chip", 0, 6, 9), ("group", 2, 3, 5))
                at(3, 5, ("chip", 3, 0, 5), ("group", 2, 5, 7))
                at(4, 0, ("chip", 3, 5, 10), ("chip", 0, 9, 10), ("group", 2, 7, 10), ("group", 0, 0, 9))
                at(4, 0, ("group", 3, 0, 10), ("group", 0, 9, 10))
                at(4, 0, ("mix", 1, 0, 5), ("mix", 0, 0, 5), ("end", 3, 2))
        else:
            for k in range(experts):
                if k + 2 < experts:
                    at(k, 2, ("z", k + 2 if inner or k else 1, 0, 5))
                if k + 1 < experts:
                    at(k, 5, ("y", k + 1, 0, 5))
                if k > 0:
                    at(k, 1, ("chip", k - 1, 0, 10))
                    at(k, 3, ("group", k - 1, 0, 10))
            at(experts, 0, ("chip", last, 0, 10), ("group", last, 0, 10))
            at(experts, 0, *[("mix", k, 0, 5) for k in range(experts - 2)])
            at(experts, 0, ("end", experts - 2, last))
        tail = ev.pop((experts, 0))
        sides.append((ev, tail))
    return sides


def kernel(
    experts,
    tok_hbm, gain_hbm, ids_hbm, mix_hbm, wg_hbm, wu_hbm, wd_hbm,
    out_ref,
    tok_ref, gain_ref, ids_ref, mix_ref, in_sem,
    wg, wu, wd, normed, disp, xin, hid, part, r1, r2s, r2r, r3s, home, acc,
    w_sem, zs_sem, zr_sem, ys_sem, yr_sem, cs_sem, cr_sem, ds_sem, dr_sem,
    r1s_sem, r1r_sem, r2s_sem, r2r_sem, r3s_sem, r3r_sem,
):
    me = lax.axis_index("ep")
    z = me // SPLIT
    y = (me // 2) % 2
    c = me % 2
    rows, width = tok_ref.shape
    cap = disp.shape[1]
    nq = cap // CHUNK
    ff = wg.shape[1]
    top = ids_ref.shape[0]
    at_y = {"ep": z * SPLIT + (1 - y) * 2 + c}
    at_c = {"ep": z * SPLIT + y * 2 + (1 - c)}
    mine = c * 2 + y
    other_y = c * 2 + 1 - y
    other_c = (1 - c) * 2 + y
    other_yc = (1 - c) * 2 + 1 - y
    near = jnp.minimum(z, experts - 1 - z)
    away = jnp.where(2 * z < experts, 1, -1)
    inner = near > 0
    edge = near == 0

    beside = min(2, experts - 1)

    def peer(k):
        from_edge = z + away * jnp.where(
            k == 0, 0, jnp.where(k == beside, 1, jnp.where(k == 1, experts - 1, experts + 1 - k))
        )
        n = jnp.where(k < 2, k, jnp.where(k == experts - 1, 2, k + 1))
        both = z + away * ((n + 1) // 2) * (2 * (n % 2) - 1)
        from_inner = jnp.where(n <= 2 * near, both, z + away * (n - near))
        return jnp.where(edge, from_edge, from_inner)

    def at_z(k):
        return {"ep": peer(k) * SPLIT + y * 2 + c}

    def remote(src, dst, send, recv, where):
        return pltpu.make_async_remote_copy(
            src_ref=src, dst_ref=dst, send_sem=send, recv_sem=recv,
            device_id=where, device_id_type=pl.DeviceIdType.MESH,
        )

    def chunk(q):
        return pl.ds(pl.multiple_of(q * CHUNK, CHUNK), CHUNK)

    ff_cuts = cut(ff, 3)
    out_cuts = cut(width, 2)
    pieces = 4

    def weight(which):
        hbm, vmem = ((wg_hbm, wg), (wu_hbm, wu), (wd_hbm, wd))[which]
        size = hbm.shape[0] // pieces
        return [
            pltpu.make_async_copy(
                hbm.at[pl.ds(i * size, size)], vmem.at[pl.ds(i * size, size)], w_sem.at[which]
            )
            for i in range(pieces)
        ]

    barrier = pltpu.get_barrier_semaphore()
    for k in range(1, experts):
        pl.semaphore_signal(barrier, inc=1, device_id=at_z(k), device_id_type=pl.DeviceIdType.MESH)
    pl.semaphore_signal(barrier, inc=1, device_id=at_y, device_id_type=pl.DeviceIdType.MESH)
    pl.semaphore_signal(barrier, inc=1, device_id=at_c, device_id_type=pl.DeviceIdType.MESH)

    inputs_in = [
        pltpu.make_async_copy(src, dst, in_sem.at[i])
        for i, (src, dst) in enumerate(
            ((ids_hbm, ids_ref), (mix_hbm, mix_ref), (gain_hbm, gain_ref), (tok_hbm, tok_ref))
        )
    ]
    for copy in inputs_in:
        copy.start()

    for copy in inputs_in:
        copy.wait()

    for which in range(3):
        for copy in weight(which):
            copy.start()

    step = tile_of(rows, 32)

    @pl.loop(0, rows // step)
    def _(r):
        at = pl.ds(pl.multiple_of(r * step, step), step)
        values = tok_ref[at, :].astype(f32)
        scale = lax.rsqrt(jnp.mean(values * values, axis=-1, keepdims=True) + 1e-06)
        normed[at, :] = (values * scale * gain_ref[...]).astype(bf16)

    lanes = 128
    expert_row = lax.broadcasted_iota(jnp.int32, (lanes, rows), 0)
    named = ids_ref[0:1, :] == expert_row
    weight_t = jnp.where(named, mix_ref[0:1, :], 0.0)
    for k in range(1, top):
        hit = ids_ref[k : k + 1, :] == expert_row
        named = named | hit
        weight_t = weight_t + jnp.where(hit, mix_ref[k : k + 1, :], 0.0)
    named = named.astype(f32)
    first = lax.broadcasted_iota(jnp.int32, (rows, rows), 0)
    second = lax.broadcasted_iota(jnp.int32, (rows, rows), 1)
    upper = (first < second).astype(f32).astype(bf16)
    rank_t = jnp.dot(named.astype(bf16), upper, preferred_element_type=f32)
    rank_t = jnp.where(named > 0.5, rank_t, -1.0)
    rank = jnp.transpose(rank_t)
    weight_c = jnp.transpose(weight_t)
    lane = lax.broadcasted_iota(jnp.int32, (rows, lanes), 1)

    def dispatch(e, dst):
        slot = jnp.sum(jnp.where(expert_row == e, rank_t, 0.0), axis=0, keepdims=True)
        place = lax.broadcasted_iota(jnp.int32, (cap, rows), 0)
        pick = (place == slot.astype(jnp.int32)).astype(f32).astype(bf16)
        wide = tile_of(width, 512)
        for n in range(width // wide):
            cols = slice(n * wide, (n + 1) * wide)
            dst[:, cols] = jnp.dot(pick, normed[:, cols], preferred_element_type=f32).astype(bf16)

    def z_copy(k, q):
        return remote(disp.at[k, chunk(q)], xin.at[z, mine, chunk(q)], zs_sem, zr_sem.at[z, q], at_z(k))

    def z_arrival(k, q):
        p = peer(k)
        return remote(disp.at[k, chunk(q)], xin.at[p, mine, chunk(q)], zs_sem, zr_sem.at[p, q], at_z(k))

    def send_z(k):
        @pl.loop(0, nq)
        def _(q):
            z_copy(k, q).start()

    def in_group(sub, send, recv, where):
        def make(k, q):
            slot = xin.at[peer(k), sub, chunk(q)]
            return remote(slot, slot, send, recv(k, q), where)

        return make

    y_copy = in_group(mine, ys_sem, lambda k, q: yr_sem.at[k, q], at_y)
    y_arrival = in_group(other_y, ys_sem, lambda k, q: yr_sem.at[k, q], at_y)
    c_copy = in_group(mine, cs_sem, lambda k, q: cr_sem.at[k], at_c)
    d_copy = in_group(other_y, ds_sem, lambda k, q: dr_sem.at[k], at_c)

    def c_arrival(k):
        slot = xin.at[peer(k), other_c]
        return remote(slot, slot, cs_sem, cr_sem.at[k], at_c)

    def d_arrival(k):
        slot = xin.at[peer(k), other_yc]
        return remote(slot, slot, ds_sem, dr_sem.at[k], at_c)

    def r1_copy(k, v, h):
        start, size = out_cuts[h]
        cols = pl.ds(start, size)
        return remote(
            part.at[k, 1 - c, v, :, cols], r1.at[k, v, :, cols], r1s_sem, r1r_sem.at[k, v, h], at_c
        )

    def piece(u):
        cols = pl.ds(pl.multiple_of(u // nq * (width // 2), width // 2), width // 2)
        return chunk(u % nq), cols

    def r2_copy(k, u):
        at = (k,) + piece(u)
        return remote(r2s.at[at], r2r.at[at], r2s_sem, r2r_sem.at[k, u], at_y)

    def r3_copy(k, u):
        at = piece(u)
        return remote(r3s.at[(k,) + at], home.at[(z,) + at], r3s_sem, r3r_sem.at[z], at_z(k))

    def r3_arrival(k):
        p = peer(k)
        return remote(r3s.at[k], home.at[p], r3s_sem, r3r_sem.at[p], at_z(k))

    def forward_z(k, q):
        if k > 0:
            z_arrival(k, q).wait_recv()
        y_copy(k, q).start()
        c_copy(k, q).start()

    def forward_y(k, q):
        y_arrival(k, q).wait_recv()
        d_copy(k, q).start()

    def r1_wait(k, v, u):
        for h in range(2):
            @pl.when(u == h * nq)
            def _():
                r1_copy(k, v, h).wait_recv()

    def chip_sum(k, u):
        at, cols = piece(u)
        r1_wait(k, 1 - y, u)
        r2s[k, at, cols] = (
            part[k, c, 1 - y, at, cols].astype(f32) + r1[k, 1 - y, at, cols].astype(f32)
        ).astype(bf16)
        r2_copy(k, u).start()

    def group_sum(k, u):
        at, cols = piece(u)
        r1_wait(k, y, u)
        r2_copy(k, u).wait_recv()
        total = (
            part[k, c, y, at, cols].astype(f32) + r1[k, y, at, cols].astype(f32) + r2r[k, at, cols].astype(f32)
        ).astype(bf16)
        if k == 0:
            home[z, at, cols] = total
        else:
            r3s[k, at, cols] = total
            r3_copy(k, u).start()

    def shares(k):
        e = peer(k)
        slot = jnp.sum(jnp.where(lane == e, rank, 0.0), axis=1, keepdims=True)
        share = jnp.sum(jnp.where(lane == e, weight_c, 0.0), axis=1, keepdims=True)
        place = lax.broadcasted_iota(jnp.int32, (rows, cap), 1)
        pick = (place == slot.astype(jnp.int32)).astype(f32).astype(bf16)
        return e, share, pick

    def mix(*blocks, last=False):
        for k in blocks:
            if k > 0:
                r3_arrival(k).wait_recv()

        parts = [shares(k) for k in blocks]
        wide = tile_of(width, 512)
        for n in range(width // wide):
            cols = slice(n * wide, (n + 1) * wide)
            total = acc[:, cols]
            for e, share, pick in parts:
                total += share * jnp.dot(pick, home[e, :, cols], preferred_element_type=f32)
            if last:
                out_ref[:, cols] = total.astype(bf16)
            else:
                acc[:, cols] = total

    actions = {"z": forward_z, "y": forward_y, "chip": chip_sum, "group": group_sum}
    sides = plan(experts, nq)

    def perform(items):
        for item in items:
            if item[0] == "mix":
                mix(item[1])
            elif item[0] == "end":
                mix(item[1], item[2], last=True)
            else:
                kind, k, lo, hi = item

                @pl.loop(lo, hi)
                def _(q):
                    actions[kind](k, q)

    def service(step_index, place):
        for k in range(experts):
            lists = [side[0].get((k, place), []) for side in sides]
            if lists[0] == lists[1]:
                if lists[0]:
                    @pl.when(step_index == k)
                    def _():
                        perform(lists[0])
            else:
                for items, kind in zip(lists, (edge, inner)):
                    if items:
                        @pl.when((step_index == k) & kind)
                        def _():
                            perform(items)

    dispatch(z, xin.at[z, mine])
    pl.semaphore_wait(barrier, experts + 1)

    @pl.loop(0, nq)
    def _(q):
        forward_z(0, q)

    @pl.loop(1, experts)
    def _(k):
        dispatch(peer(k), disp.at[k])

        @pl.when(jnp.where(inner, (k == 1) | (k == experts - 1), k == beside))
        def _():
            send_z(k)

    acc[...] = jnp.zeros_like(acc)

    def forward_near(q):
        @pl.when(inner)
        def _():
            forward_z(1, q)

        @pl.when(edge)
        def _():
            forward_z(beside, q)

    lead = min(2, nq)

    @pl.loop(0, lead)
    def _(q):
        forward_y(0, q)

    @pl.loop(lead, nq)
    def _(q):
        forward_near(q - lead)
        forward_y(0, q)

    @pl.loop(nq - lead, nq)
    def _(q):
        forward_near(q)

    @pl.loop(1, experts)
    def _(k):
        @pl.when(jnp.where(inner, (k > 1) & (k < experts - 1), k != beside))
        def _():
            send_z(k)

    for which, (hbm, vmem) in enumerate(((wg_hbm, wg), (wu_hbm, wu), (wd_hbm, wd))):
        pltpu.make_async_copy(hbm, vmem, w_sem.at[which]).wait()

    @pl.loop(0, experts)
    def _(k):
        c_arrival(k).wait_recv()
        d_arrival(k).wait_recv()

        for h, (start, size) in enumerate(ff_cuts):
            cols = slice(start, start + size)
            inputs = xin[peer(k)].reshape(SPLIT * cap, width)
            gate = jnp.dot(inputs, wg[:, cols], preferred_element_type=f32)
            up = jnp.dot(inputs, wu[:, cols], preferred_element_type=f32)
            hid[:, cols] = (gate / (1.0 + jnp.exp(-gate)) * up).astype(bf16)
            service(k, 1 + h)

        for h, (start, size) in enumerate(out_cuts):
            cols = slice(start, start + size)
            res = jnp.dot(hid[...], wd[:, cols], preferred_element_type=f32).astype(bf16)
            part[k, :, :, :, cols] = res.reshape(2, 2, cap, size)
            for v in (1 - y, y):
                r1_copy(k, v, h).start()
            service(k, 1 + len(ff_cuts) + h)

    tails = [side[1] for side in sides]
    if tails[0] == tails[1]:
        perform(tails[0])
    else:
        for items, kind in zip(tails, (edge, inner)):
            @pl.when(kind)
            def _():
                perform(items)


    others = pl.ds(1, experts - 1)
    remote(disp.at[others], disp.at[others], zs_sem, cr_sem.at[0], at_c).wait_send()
    remote(disp, disp, ys_sem, cr_sem.at[0], at_c).wait_send()
    remote(disp, disp, cs_sem, cr_sem.at[0], at_c).wait_send()
    remote(disp, disp, ds_sem, cr_sem.at[0], at_c).wait_send()
    remote(part.at[:, 0], r1, r1s_sem, cr_sem.at[0], at_c).wait_send()
    remote(r2s, r2r, r2s_sem, cr_sem.at[0], at_c).wait_send()
    remote(r3s.at[others], home.at[others], r3s_sem, cr_sem.at[0], at_c).wait_send()


def local(tokens, norm_gain, expert_ids, mix_weights, gate_weight, up_weight, down_weight):
    n_dev = lax.axis_size("ep")
    experts = n_dev // SPLIT
    rows, width = tokens.shape
    top = expert_ids.shape[1]
    ff = gate_weight.shape[1]
    cap = (rows * top * SPLIT * 5 + 4 * n_dev - 1) // (4 * n_dev)
    cap = (cap + CHUNK - 1) // CHUNK * CHUNK
    nq = cap // CHUNK
    dma = pltpu.SemaphoreType.DMA
    vmem = pl.BlockSpec(memory_space=pltpu.VMEM)
    hbm = pl.BlockSpec(memory_space=pl.ANY)
    block = (cap, width)
    return pl.pallas_call(
        functools.partial(kernel, experts),
        out_shape=pltpu.VMEM((rows, width), bf16),
        in_specs=[hbm] * 7,
        out_specs=vmem,
        scratch_shapes=[
            pltpu.VMEM((rows, width), bf16),
            pltpu.VMEM((1, width), f32),
            pltpu.VMEM((top, rows), jnp.int32),
            pltpu.VMEM((top, rows), f32),
            dma((4,)),
            pltpu.VMEM((width, ff), bf16),
            pltpu.VMEM((width, ff), bf16),
            pltpu.VMEM((ff, width), bf16),
            pltpu.VMEM((rows, width), bf16),
            pltpu.VMEM((experts,) + block, bf16),
            pltpu.VMEM((experts, SPLIT) + block, bf16),
            pltpu.VMEM((SPLIT * cap, ff), bf16),
            pltpu.VMEM((experts, 2, 2) + block, bf16),
            pltpu.VMEM((experts, 2) + block, bf16),
            pltpu.VMEM((experts,) + block, bf16),
            pltpu.VMEM((experts,) + block, bf16),
            pltpu.VMEM((experts,) + block, bf16),
            pltpu.VMEM((experts,) + block, bf16),
            pltpu.VMEM((rows, width), f32),
            dma((3,)),
                    dma, dma((experts, nq)), dma, dma((experts, nq)), dma, dma((experts,)), dma, dma((experts,)),
            dma, dma((experts, 2, 2)), dma, dma((experts, 2 * nq)), dma, dma((experts,)),
        ],
        compiler_params=pltpu.CompilerParams(
            collective_id=0, has_side_effects=True, vmem_limit_bytes=58 * 1024 * 1024,
        ),
    )(tokens, norm_gain.reshape(1, width), expert_ids.T, mix_weights.T, gate_weight, up_weight, down_weight)


def solution(mesh):
    in_specs = (
        P(("grp", "ep"), None),
        P(),
        P(("grp", "ep"), None),
        P(("grp", "ep"), None),
        P(None, "ep"),
        P(None, "ep"),
        P("ep", None),
    )
    out_specs = P(("grp", "ep"), None)
    return jax.shard_map(local, mesh=mesh, in_specs=in_specs, out_specs=out_specs, check_vma=False)
```
